32 devices in a mesh: ep: 8 (over z, y), tp: 4 (over x, core).
Axes of the slice: x: 2, y: 2, z: 4, core: 2. Of those that a mesh axis runs over, the one named last changes fastest.
Arguments:
- first_input: bfloat16 [4096, 2048], P('ep'), may hold values from -120 to 120
- first_gain: bfloat16 [2048], replicated, may hold values from 0.099609375 to 1.8984375
- pool_inward: bfloat16 [2048, 1024], P(None, 'tp'), may hold values from -0.125 to 0.125
- pool_mixing: bfloat16 [4, 256, 256], P('tp'), may hold values from -0.375 to 0.375
- pool_scale: bfloat16 [1024], P('tp'), may hold values from 0.099609375 to 1.8984375
- pool_outward: bfloat16 [1024, 2048], P('tp'), may hold values from -0.1875 to 0.1875
- second_input: bfloat16 [2048, 2048], P('ep'), may hold values from -120 to 120
- second_gain: bfloat16 [2048], replicated, may hold values from 0.099609375 to 1.8984375
- route_ids: int32 [2048, 2], P('ep'), may hold values from 0 to 3, all different within a row; in each aligned block of 256 rows (0 to 255, 256 to 511, ...) at most 144 rows name the same one
- route_logits: float32 [2048, 2], P('ep'), may hold values from -6 to 6
- expert_gate: bfloat16 [8, 2048, 2048], P('ep', None, 'tp'), may hold values from -0.125 to 0.125
- expert_up: bfloat16 [8, 2048, 2048], P('ep', None, 'tp'), may hold values from -0.125 to 0.125
- expert_down: bfloat16 [8, 2048, 2048], P('ep', 'tp'), may hold values from -0.09375 to 0.09375
Outputs:
- first_out: bfloat16 [4096, 2048], P('ep', 'tp')
- second_out: bfloat16 [2048, 2048], P('ep', 'tp')
The draws below stay inside these ranges and needn't reach their ends.
Inputs may be any that keep to these rules, and one draw needn't show every extreme that they name: `route_ids`: each row names two different experts. In each aligned block of 256 rows (the rows of one index of ep) no expert is named by more than 144 rows, and in some blocks one expert is named by exactly 144 rows.
All inputs are finite; a program needn't handle non-finite values.
Results may differ from the reference program's by a relative error of at most 0.012.
Values may be sent and summed in bfloat16 or wider, within the bound.
A program may use at most 64 MiB of HBM per device.

```python
import math
import jax
import jax.numpy as jnp
import numpy as np
from jax import lax

D = 2048
POOL = 1024
FF_E = 4096
B_ROWS = 256
EXPERTS = 4
CAP = 144
TOK_A = 4096
TOK_B = 2048
N_EP = 8
N_TP = 4


def scaled_rows(key, row_count, width):
    subkeys = jax.random.split(key, 3)
    column_scale = jnp.exp(jax.random.uniform(subkeys[1], (1, width), jnp.float32, 0.0, math.log(10.0)))
    row_scale = jnp.exp(jax.random.uniform(subkeys[2], (row_count, 1), jnp.float32, 0.0, math.log(10.0)))
    values = jax.random.truncated_normal(subkeys[0], -4.0, 4.0, (row_count, width), jnp.float32)
    return (values * column_scale * row_scale * 0.25).astype(jnp.bfloat16)


def draw_first_input(key, part):
    return scaled_rows(jax.random.fold_in(key, 11), TOK_A, D)


def draw_second_input(key, part):
    return scaled_rows(jax.random.fold_in(key, 23), TOK_B, D)


def levels(own_key, extent, cuts, least, high):
    def one(position, blocks):
        steps = jax.random.uniform(jax.random.fold_in(jax.random.fold_in(own_key, 6), position), (blocks,), jnp.float32, least / len(cuts), high / len(cuts))
        return jnp.repeat(jnp.exp(steps), extent[position] // blocks).reshape((-1,) + (1,) * (len(extent) - position - 1))

    loudness = one(*cuts[0])
    for cut in cuts[1:]:
        loudness = loudness * one(*cut)
    return loudness


def assign_block(rng, own, number, rows, amount, top, reach, skew):
    order = jax.random.permutation(rng, amount)
    packed, ordinary = portions_of(amount, rows * top, reach, skew, True), portions_of(amount, rows * top, reach, skew, False)
    places = jnp.arange(amount)

    def named(tallies, turn):
        used = int((tallies > 0).sum())
        fixed = max(1, used // 4)
        shifted = fixed + (places - fixed + turn * (used - fixed)) % max(1, amount - fixed)
        return jnp.zeros((amount,), jnp.int32).at[order[jnp.where(places < fixed, places, shifted)]].set(jnp.asarray(tallies, jnp.int32))

    tallies = jnp.where(number % 4 == 0, named(packed, number // 4), named(ordinary, number - number // 4 - 1))
    mixed = jax.random.permutation(jax.random.fold_in(own, 3), amount)
    donor, sink = mixed[0:amount // 2 * 2:2], mixed[1:amount // 2 * 2:2]
    slack = jnp.minimum(tallies[donor] - 1, reach - tallies[sink]) // 2
    slack = jnp.where((donor == order[0]) | (sink == order[0]) | (tallies[sink] == 0), 0, jnp.maximum(slack, 0))
    shifted = jax.random.randint(jax.random.fold_in(own, 4), (amount // 2,), 0, 1 << 20) % (slack + 1)
    tallies = tallies.at[donor].add(-shifted).at[sink].add(shifted)
    items = jnp.searchsorted(jnp.cumsum(tallies), jnp.arange(rows * top), side="right").astype(jnp.int32)
    listing = items.reshape(top, rows).T
    listing = listing[jax.random.permutation(jax.random.fold_in(own, 1), rows)]
    turn = jax.random.randint(jax.random.fold_in(own, 2), (rows, 1), 0, top)
    return jnp.take_along_axis(listing, (jnp.arange(top)[None, :] + turn) % top, axis=1)


def portions_of(count, total, most, slope, full):
    portions = [(1 << 20) // math.isqrt(grade ** slope) + 1 for grade in range(1, count + 1)]
    largest = most if full else min(most, max(-(-total // count), total * portions[0] // sum(portions)))
    least = 1 if total - largest >= count - 1 else 0
    given, surplus = [largest] + [least] * (count - 1), total - largest - least * (count - 1)
    while surplus > 0:
        free = [i for i in range(1, count) if given[i] < largest] or [i for i in range(1, count) if given[i] < most]
        whole, left = sum([portions[i] for i in free]), surplus
        for i in free:
            extra = min(most - given[i], max(1, left * portions[i] // whole), surplus)
            given[i] = given[i] + extra
            surplus = surplus - extra
    return np.array(given)


def noise(rng, extent, scale, most, pieces=(), kind=jnp.bfloat16):
    array = scale * jax.random.normal(rng, extent, jnp.float32)
    if pieces:
        array = array * levels(rng, extent, pieces, -0.22, 0.18)
    return jnp.clip(array, -most, most).astype(kind)


def setup_inputs(seed: int = 0) -> dict:
    seeds = jax.random.split(jax.random.key(seed), 14)
    first_input = draw_first_input(jax.random.fold_in(seeds[13], 71), 0)
    first_gain = jnp.clip(1.0 + 0.18 * jax.random.normal(seeds[1], (D,), jnp.float32), 0.099609375, 1.8984375).astype(jnp.bfloat16)
    pool_inward = noise(seeds[2], (D, POOL), D ** -0.5, 0.125, ((1, 4),))
    pool_mixing = noise(seeds[3], (4, POOL // 4, POOL // 4), (POOL // 4) ** -0.5, 0.375, ((0, 4),))
    pool_scale = jnp.clip(1.0 + 0.18 * jax.random.normal(seeds[4], (POOL,), jnp.float32), 0.099609375, 1.8984375).astype(jnp.bfloat16)
    pool_outward = noise(seeds[5], (POOL, D), POOL ** -0.5, 0.1875, ((0, 4),))
    second_input = draw_second_input(jax.random.fold_in(seeds[13], 71), 0)
    second_gain = jnp.clip(1.0 + 0.18 * jax.random.normal(seeds[7], (D,), jnp.float32), 0.099609375, 1.8984375).astype(jnp.bfloat16)
    route_ids_keys = jax.random.split(jax.random.fold_in(seeds[8], 1), TOK_B // B_ROWS)
    route_ids_turns = jax.random.permutation(jax.random.fold_in(seeds[8], 3), TOK_B // B_ROWS)
    route_ids = jax.vmap(lambda own, number: assign_block(jax.random.fold_in(seeds[8], 2), own, number, B_ROWS, EXPERTS, 2, CAP, 0))(route_ids_keys, route_ids_turns).reshape((TOK_B, 2))
    route_logits = noise(seeds[9], (TOK_B, 2), 1.5, 6.0, ((0, 8),), jnp.float32)
    expert_gate = noise(seeds[10], (2 * EXPERTS, D, FF_E // 2), D ** -0.5, 0.125, ((0, 8), (2, 4)))
    expert_up = noise(seeds[11], (2 * EXPERTS, D, FF_E // 2), D ** -0.5, 0.125, ((0, 8), (2, 4)))
    expert_down = noise(seeds[12], (2 * EXPERTS, FF_E // 2, D), FF_E ** -0.5, 0.09375, ((0, 8), (1, 4)))
    return dict(first_input=first_input, first_gain=first_gain, pool_inward=pool_inward, pool_mixing=pool_mixing, pool_scale=pool_scale, pool_outward=pool_outward, second_input=second_input, second_gain=second_gain, route_ids=route_ids, route_logits=route_logits, expert_gate=expert_gate, expert_up=expert_up, expert_down=expert_down)


epsilon = 1e-06
window_lengths = (2, 4, 8, 16)

def rms_scaled(values, weights):
    widened = values.astype(jnp.float32)
    inverse = lax.rsqrt(lax.optimization_barrier(jnp.mean(widened * widened, axis=-1, keepdims=True)) + epsilon)
    return (widened * inverse * weights.astype(jnp.float32)).astype(jnp.bfloat16)

def window_means(channels, length, offset):
    row_count = channels.shape[0] - 15
    summed = jnp.zeros((row_count, channels.shape[1]), jnp.float32)
    for lookback in range(16):
        summed = summed + jnp.where(lookback < length, channels[15 - lookback:15 - lookback + row_count], 0.0)
    positions = offset + jnp.arange(row_count, dtype=jnp.int32)
    counts = jnp.minimum(positions + 1, length).astype(jnp.float32)
    return summed / counts[:, None]

def slot_positions(block_ids, expert_count, capacity):
    flattened = block_ids.reshape(-1)
    onehot = (flattened[:, None] == jnp.arange(expert_count, dtype=jnp.int32)[None, :]).astype(jnp.int32)
    running = jnp.cumsum(onehot, axis=0, dtype=jnp.int32) - 1
    slot_numbers = lax.optimization_barrier(jnp.sum(onehot * running, axis=1))
    return (flattened * capacity + slot_numbers).astype(jnp.int32)

def mixer_half(first_input, first_gain, pool_inward, pool_mixing, pool_scale, pool_outward):
    normed = rms_scaled(first_input, first_gain)
    pooled_in = jnp.dot(normed, pool_inward, preferred_element_type=jnp.float32).astype(jnp.bfloat16)
    group_width = pool_inward.shape[1] // 4
    accumulated = jnp.zeros(first_input.shape, jnp.float32)
    for group_index in range(4):
        lower = group_index * group_width
        channels = pooled_in[:, lower:lower + group_width]
        widened = jnp.pad(channels.astype(jnp.float32), ((15, 0), (0, 0)))
        means = window_means(widened, window_lengths[group_index], jnp.int32(0))
        mixed = (means - channels.astype(jnp.float32)).astype(jnp.bfloat16)
        scales = pool_scale[lower:lower + group_width].astype(jnp.float32)
        pooled = (jnp.dot(mixed, pool_mixing[group_index], preferred_element_type=jnp.float32) * scales).astype(jnp.bfloat16)
        partial_value = jnp.dot(pooled, pool_outward[lower:lower + group_width], preferred_element_type=jnp.float32).astype(jnp.bfloat16)
        accumulated = accumulated + partial_value.astype(jnp.float32)
    return accumulated.astype(jnp.bfloat16)

def block_tables(block_positions, block_shares, first_token):
    tokens = first_token + jnp.arange(2 * B_ROWS, dtype=jnp.int32) // 2
    owners = jnp.zeros((EXPERTS * CAP,), jnp.int32).at[block_positions].set(tokens)
    weights = jnp.zeros((EXPERTS * CAP,), jnp.float32).at[block_positions].set(block_shares)
    return (owners, weights)

def block_slots(block_ids):
    return slot_positions(block_ids, EXPERTS, CAP)

def expert_half(second_input, second_gain, route_ids, route_logits, expert_gate, expert_up, expert_down):
    normed = rms_scaled(second_input, second_gain)
    positions = jax.vmap(block_slots)(route_ids.reshape(N_EP, B_ROWS, 2))
    shares = jax.nn.sigmoid(route_logits - route_logits[:, ::-1])
    starts = jnp.arange(N_EP, dtype=jnp.int32) * B_ROWS
    owners, weights = jax.vmap(block_tables)(positions, shares.reshape(N_EP, 2 * B_ROWS), starts)
    owners = owners.reshape(N_EP, EXPERTS, CAP).transpose(1, 0, 2).reshape(EXPERTS, N_EP * CAP)
    weights = weights.reshape(N_EP, EXPERTS, CAP).transpose(1, 0, 2).reshape(EXPERTS, N_EP * CAP)
    half_units = expert_gate.shape[2]
    unit_group = half_units // N_TP
    gate_pairs = expert_gate.reshape(EXPERTS, 2, D, half_units)
    up_pairs = expert_up.reshape(EXPERTS, 2, D, half_units)
    down_pairs = expert_down.reshape(EXPERTS, 2, half_units, D)

    def add_expert(accumulated, inputs):
        slot_owners, slot_weights, gate_pair, up_pair, down_pair = inputs
        routed = normed[slot_owners]
        gate_full = jnp.concatenate([gate_pair[0], gate_pair[1]], axis=1)
        up_full = jnp.concatenate([up_pair[0], up_pair[1]], axis=1)
        gate_sum = jnp.dot(routed, gate_full, preferred_element_type=jnp.float32)
        up_sum = jnp.dot(routed, up_full, preferred_element_type=jnp.float32)
        hidden = (jax.nn.silu(gate_sum) * up_sum).astype(jnp.bfloat16)
        down_full = down_pair.reshape(2 * half_units, D)
        route_out = jnp.zeros((routed.shape[0], D), jnp.float32)
        for half_index in range(2):
            half_sum = jnp.zeros((routed.shape[0], D), jnp.float32)
            for quarter in range(N_TP):
                first_unit = half_index * half_units + quarter * unit_group
                product = jnp.dot(hidden[:, first_unit:first_unit + unit_group], down_full[first_unit:first_unit + unit_group], preferred_element_type=jnp.float32).astype(jnp.bfloat16)
                half_sum = half_sum + product.astype(jnp.float32)
            route_out = route_out + half_sum.astype(jnp.bfloat16).astype(jnp.float32)
        return (accumulated.at[slot_owners].add(slot_weights[:, None] * route_out), None)
    accumulated, unused = lax.scan(add_expert, jnp.zeros((second_input.shape[0], D), jnp.float32), (owners, weights, gate_pairs, up_pairs, down_pairs))
    return accumulated.astype(jnp.bfloat16)

def reference(first_input, first_gain, pool_inward, pool_mixing, pool_scale, pool_outward, second_input, second_gain, route_ids, route_logits, expert_gate, expert_up, expert_down):
    first_out = mixer_half(first_input, first_gain, pool_inward, pool_mixing, pool_scale, pool_outward)
    second_out = expert_half(second_input, second_gain, route_ids, route_logits, expert_gate, expert_up, expert_down)
    return (first_out, second_out)
```

```python
import functools

import jax
import jax.numpy as jnp
from jax import lax
from jax.experimental import pallas as pl
from jax.experimental.pallas import tpu as pltpu
from jax.sharding import PartitionSpec as P

EPS = 1e-06
MESH = pl.DeviceIdType.MESH
F32, BF16 = jnp.float32, jnp.bfloat16


def ring_order(n):
    order = [0]
    for step in range(1, n // 2 + 1):
        order.append(step)
        if n - step != step:
            order.append(n - step)
    return order


def rms(values, gain):
    wide = values.astype(F32)
    inverse = lax.rsqrt(jnp.mean(wide * wide, axis=-1, keepdims=True) + EPS)
    return (wide * inverse * gain).astype(BF16)


def body(
    n, parts, cap,
    first_hbm, gain1, inward_hbm, mixing, scale, outward_hbm, x2, gain2, ids, ids_t, logits,
    gate_hbm, up_hbm, down_hbm,
    out1, out2,
    first_v, inward_v, outward_v, gate_v, up_v, down_v, load_sem,
    normed, sent, portion, hidden, term, core_in, x_out, x_in, half_out, back, total,
    halo_out, halo_in, extended, mixed, pooled, mix_term, mix_core, mix_x_out, mix_x_in,
    z_send, z_recv, xs, xr, d1s, d1r, d2s, d2r,
    r1s, r1r, r2s, r2r, r3s, r3r, hs, hr, m1s, m1r, m2s, m2r,
):
    me = lax.axis_index("ep")
    t = lax.axis_index("tp")
    t_core = t + 1 - 2 * lax.rem(t, 2)
    t_x = lax.rem(t + 2, 4)
    t_diag = lax.rem(t_core + 2, 4)
    rows2, width = x2.shape
    w = width // parts
    order = ring_order(n)
    groups = 4
    per = n // groups
    group_rows = per * cap
    rows1 = first_v.shape[0]
    tile1 = 128

    def quarter(index):
        return pl.ds(pl.multiple_of(index * w, w), w)

    def spot(i):
        return pl.ds(i * cap, cap)

    def group(g):
        return pl.ds(g * group_rows, group_rows)

    loads = [
        pltpu.make_async_copy(src, dst, load_sem.at[k])
        for k, (src, dst) in enumerate((
            (first_hbm, first_v), (inward_hbm, inward_v), (outward_hbm, outward_v),
            (gate_hbm.at[0], gate_v), (up_hbm.at[0], up_v), (down_hbm.at[0], down_v)))
    ]
    for load in loads:
        load.start()

    barrier = pltpu.get_barrier_semaphore()
    for r in range(1, n):
        pl.semaphore_signal(barrier, inc=1, device_id=(lax.rem(me + r, n), t), device_id_type=MESH)
    for other in (t_core, t_x):
        pl.semaphore_signal(barrier, inc=1, device_id=(me, other), device_id_type=MESH)

    def remote(src, dst, ssem, rsem, ep, tp):
        return pltpu.make_async_remote_copy(
            src_ref=src, dst_ref=dst, send_sem=ssem, recv_sem=rsem,
            device_id=(ep, tp), device_id_type=MESH)

    def z_copy(i):
        return remote(sent.at[spot(i)], portion.at[spot(i), quarter(t)],
                      z_send.at[i], z_recv.at[i], lax.rem(me + order[i], n), t)

    def x_copy(i):
        piece = portion.at[spot(i), quarter(t)]
        return remote(piece, piece, xs.at[i], xr.at[i], me, t_x)

    def x_arrival(i):
        piece = portion.at[spot(i), quarter(t_x)]
        return remote(piece, piece, xs.at[i], xr.at[i], me, t_x)

    def d1_copy(i):
        piece = portion.at[spot(i), quarter(t)]
        return remote(piece, piece, d1s.at[i], d1r.at[i], me, t_core)

    def d1_arrival(i):
        piece = portion.at[spot(i), quarter(t_core)]
        return remote(piece, piece, d1s.at[i], d1r.at[i], me, t_core)

    def d2_copy(i):
        piece = portion.at[spot(i), quarter(t_x)]
        return remote(piece, piece, d2s.at[i], d2r.at[i], me, t_core)

    def d2_arrival(i):
        piece = portion.at[spot(i), quarter(t_diag)]
        return remote(piece, piece, d2s.at[i], d2r.at[i], me, t_core)

    def r1_copy(g, k):
        return remote(term.at[group(g), quarter((t_core, t_diag)[k])], core_in.at[k, group(g)],
                      r1s.at[g, k], r1r.at[g, k], me, t_core)

    def r2_copy(g):
        return remote(x_out.at[group(g)], x_in.at[group(g)], r2s.at[g], r2r.at[g], me, t_x)

    def r3_copy(i):
        return remote(half_out.at[spot(i)], back.at[spot(i)], r3s.at[i], r3r.at[i],
                      lax.rem(me + n - order[i], n), t)

    def m1_copy(k):
        return remote(mix_term.at[:, quarter((t_core, t_diag)[k])], mix_core.at[k],
                      m1s.at[k], m1r.at[k], me, t_core)

    def m2_copy():
        return remote(mix_x_out, mix_x_in, m2s, m2r, me, t_x)

    def halo_copy():
        return remote(halo_out, halo_in, hs, hr, lax.rem(me + 1, n), t)

    def norm_tile(j, carry):
        tile = pl.ds(pl.multiple_of(j * 64, 64), 64)
        normed[tile, :] = rms(x2[tile, :], gain2[...].astype(F32))
        return carry

    lax.fori_loop(0, rows2 // 64, norm_tile, None)

    before = (lax.broadcasted_iota(jnp.int32, (rows2, rows2), 0)
              < lax.broadcasted_iota(jnp.int32, (rows2, rows2), 1)).astype(BF16)
    places = lax.broadcasted_iota(jnp.int32, (cap, rows2), 0)

    def chosen(i):
        expert = lax.rem(me + order[i], n) // 2
        named = (ids_t[0:1, :] == expert) | (ids_t[1:2, :] == expert)
        flags = jnp.broadcast_to(jnp.where(named, 1.0, 0.0), (16, rows2)).astype(BF16)
        slots = jnp.dot(flags, before, preferred_element_type=F32)[0:1, :].astype(jnp.int32)
        slots = jnp.where(named, slots, -1)
        return jnp.where(places == slots, 1.0, 0.0).astype(BF16)

    pl.semaphore_wait(barrier, n + 1)
    for i in range(1, n):
        sent[spot(i), :] = jnp.dot(
            chosen(i), normed[:, quarter(t)], preferred_element_type=F32).astype(BF16)
        z_copy(i).start()
    own_rows = chosen(0)
    for q in range(parts):
        portion[spot(0), q * w:(q + 1) * w] = jnp.dot(
            own_rows, normed[:, q * w:(q + 1) * w], preferred_element_type=F32).astype(BF16)

    loads[0].wait()
    loads[1].wait()

    def inward_tile(j, carry):
        tile = pl.ds(pl.multiple_of(j * tile1, tile1), tile1)
        later = pl.ds(pl.multiple_of(j * tile1 + 16, 16), tile1)
        rows = rms(first_v[tile, :], gain1[...].astype(F32))
        product = jnp.dot(rows, inward_v[...], preferred_element_type=F32).astype(BF16)
        extended[later, :] = product.astype(F32)
        return carry

    lax.fori_loop(0, rows1 // tile1, inward_tile, None)
    halo_out[...] = extended[rows1:rows1 + 16, :].astype(BF16)
    halo_copy().start()

    def relay1(i):
        z_copy(i).wait_recv()
        x_copy(i).start()
        d1_copy(i).start()

    def relay2(i):
        x_arrival(i).wait_recv()
        d2_copy(i).start()

    def ready(i):
        d1_arrival(i).wait_recv()
        d2_arrival(i).wait_recv()

    def positions(g):
        return [i for i in range(g * per, (g + 1) * per) if i > 0]

    def relay(step, g):
        if g < groups:
            for i in positions(g):
                step(i)

    def compute(g):
        unit_tile = min(256, hidden.shape[1])

        def units(j, carry):
            cols = pl.ds(pl.multiple_of(j * unit_tile, unit_tile), unit_tile)
            gate = jnp.dot(portion[group(g), :], gate_v[:, cols], preferred_element_type=F32)
            up = jnp.dot(portion[group(g), :], up_v[:, cols], preferred_element_type=F32)
            hidden[:, cols] = (gate / (1.0 + jnp.exp(-gate)) * up).astype(BF16)
            return carry

        lax.fori_loop(0, hidden.shape[1] // unit_tile, units, None)

        def outs(j, carry):
            cols = quarter(j)
            term[group(g), cols] = jnp.dot(
                hidden[...], down_v[:, cols], preferred_element_type=F32).astype(BF16)
            return carry

        lax.fori_loop(0, parts, outs, None)
        for k in (1, 0):
            r1_copy(g, k).start()

    def over_x(g):
        r1_copy(g, 1).wait_recv()
        x_out[group(g), :] = (term[group(g), quarter(t_x)].astype(F32)
                              + core_in[1, group(g), :].astype(F32)).astype(BF16)
        r2_copy(g).start()

    def home(g):
        r1_copy(g, 0).wait_recv()
        r2_copy(g).wait_recv()
        half_out[group(g), :] = (term[group(g), quarter(t)].astype(F32)
                                 + core_in[0, group(g), :].astype(F32)
                                 + x_in[group(g), :].astype(F32)).astype(BF16)
        for i in positions(g):
            r3_copy(i).start()

    relay(relay1, 0)

    halo_copy().wait_recv()
    loads[2].wait()
    extended[0:16, :] = jnp.where(me == 0, 0.0, halo_in[...].astype(F32))
    lanes = min(128, extended.shape[1])
    counts = jnp.minimum(
        me * rows1 + 1 + lax.broadcasted_iota(jnp.int32, (rows1, lanes), 0),
        jnp.left_shift(jnp.int32(2), t)).astype(F32)
    for c in range(extended.shape[1] // lanes):
        cols = slice(c * lanes, (c + 1) * lanes)
        whole = extended[:, cols]
        running, picked = whole, whole
        for level in range(4):
            running = running + pltpu.roll(running, 1 << level, 0)
            picked = jnp.where(t >= level, running, picked)
        mixed[:, cols] = (picked[16:, :] / counts - whole[16:, :]).astype(BF16)
    pooled[...] = (jnp.dot(mixed[...], mixing[0], preferred_element_type=F32)
                   * scale[...].astype(F32)).astype(BF16)

    def outward_tile(j, carry):
        mix_term[:, quarter(j)] = jnp.dot(
            pooled[...], outward_v[:, quarter(j)], preferred_element_type=F32).astype(BF16)
        return carry

    lax.fori_loop(0, parts, outward_tile, None)
    m1_copy(1).start()
    m1_copy(0).start()

    relay(relay2, 0)
    relay(relay1, 1)
    m1_copy(1).wait_recv()
    mix_x_out[...] = (mix_term[:, quarter(t_x)].astype(F32)
                      + mix_core[1].astype(F32)).astype(BF16)
    m2_copy().start()
    for k in (3, 4, 5):
        loads[k].wait()
    relay(ready, 0)
    compute(0)
    relay(relay2, 1)
    relay(relay1, 2)
    over_x(0)
    relay(ready, 1)
    compute(1)
    relay(relay2, 2)
    relay(relay1, 3)
    over_x(1)
    home(0)
    relay(ready, 2)
    compute(2)
    relay(relay2, 3)
    over_x(2)
    home(1)
    relay(ready, 3)
    compute(3)
    over_x(3)
    home(2)

    m1_copy(0).wait_recv()
    m2_copy().wait_recv()
    out1[...] = (mix_term[:, quarter(t)].astype(F32) + mix_core[0].astype(F32)
                 + mix_x_in[...].astype(F32)).astype(BF16)

    after = (lax.broadcasted_iota(jnp.int32, (rows2, rows2), 1)
             < lax.broadcasted_iota(jnp.int32, (rows2, rows2), 0)).astype(BF16)
    tall = lax.broadcasted_iota(jnp.int32, (rows2, cap), 1)
    difference = logits[:, 0:1] - logits[:, 1:2]
    share0 = 1.0 / (1.0 + jnp.exp(-difference))
    share1 = 1.0 / (1.0 + jnp.exp(difference))

    def combine(i, source):
        expert = lax.rem(me + order[i], n) // 2
        is0, is1 = ids[:, 0:1] == expert, ids[:, 1:2] == expert
        named = is0 | is1
        flags = jnp.broadcast_to(jnp.where(named, 1.0, 0.0), (rows2, 128)).astype(BF16)
        slots = jnp.dot(after, flags, preferred_element_type=F32)[:, 0:1].astype(jnp.int32)
        slots = jnp.where(named, slots, -1)
        table = jnp.where(tall == slots, 1.0, 0.0).astype(BF16)
        share = jnp.where(is0, share0, jnp.where(is1, share1, 0.0))
        picked = share * jnp.dot(table, source[spot(i), :], preferred_element_type=F32)
        if i == 0:
            total[...] = picked
        else:
            total[...] += picked

    def gather(g):
        for i in positions(g):
            r3_copy(i).wait_recv()
            combine(i, back)

    combine(0, half_out)
    gather(0)
    gather(1)
    home(3)
    gather(2)
    gather(3)
    out2[...] = total[...].astype(BF16)

    for i in range(1, n):
        z_copy(i).wait_send()
        x_copy(i).wait_send()
        d1_copy(i).wait_send()
        d2_copy(i).wait_send()
        r3_copy(i).wait_send()
    for g in range(groups):
        r1_copy(g, 0).wait_send()
        r1_copy(g, 1).wait_send()
        r2_copy(g).wait_send()
    m1_copy(0).wait_send()
    m1_copy(1).wait_send()
    m2_copy().wait_send()
    halo_copy().wait_send()


def local(
    first_input, first_gain, pool_inward, pool_mixing, pool_scale, pool_outward,
    second_input, second_gain, route_ids, route_logits, expert_gate, expert_up, expert_down,
):
    n = lax.axis_size("ep")
    parts = lax.axis_size("tp")
    experts = n // 2
    rows1, width = first_input.shape
    rows2 = second_input.shape[0]
    w = width // parts
    cap = 2 * rows2 * 9 // (8 * experts)
    cap = -(-cap // 16) * 16
    channels = pool_inward.shape[1]
    units = expert_gate.shape[2]
    slots = n * cap
    dma = pltpu.SemaphoreType.DMA
    vmem = pl.BlockSpec(memory_space=pltpu.VMEM)
    anywhere = pl.BlockSpec(memory_space=pl.ANY)
    v = pltpu.VMEM
    scratch = [
        v((rows1, width), BF16), v((width, channels), BF16), v((channels, width), BF16),
        v((width, units), BF16), v((width, units), BF16), v((units, width), BF16), dma((6,)),
        v((rows2, width), BF16), v((slots, w), BF16), v((slots, width), BF16),
        v((slots // 4, units), BF16), v((slots, width), BF16), v((2, slots, w), BF16),
        v((slots, w), BF16), v((slots, w), BF16), v((slots, w), BF16), v((slots, w), BF16),
        v((rows2, w), F32),
        v((16, channels), BF16), v((16, channels), BF16), v((rows1 + 16, channels), F32),
        v((rows1, channels), BF16), v((rows1, channels), BF16), v((rows1, width), BF16),
        v((2, rows1, w), BF16), v((rows1, w), BF16), v((rows1, w), BF16),
        dma((n,)), dma((n,)), dma((n,)), dma((n,)), dma((n,)), dma((n,)), dma((n,)), dma((n,)),
        dma((4, 2)), dma((4, 2)), dma((4,)), dma((4,)), dma((n,)), dma((n,)),
        dma(()), dma(()), dma((2,)), dma((2,)), dma(()), dma(()),
    ]
    return pl.pallas_call(
        functools.partial(body, n, parts, cap),
        out_shape=(jax.ShapeDtypeStruct((rows1, w), BF16), jax.ShapeDtypeStruct((rows2, w), BF16)),
        in_specs=[anywhere, vmem, anywhere, vmem, vmem, anywhere, vmem, vmem, vmem, vmem, vmem,
                  anywhere, anywhere, anywhere],
        out_specs=(vmem, vmem),
        scratch_shapes=scratch,
        compiler_params=pltpu.CompilerParams(
            collective_id=0, has_side_effects=True, vmem_limit_bytes=60 * 1024 * 1024),
    )(
        first_input, first_gain[None, :], pool_inward, pool_mixing, pool_scale[None, :],
        pool_outward, second_input, second_gain[None, :], route_ids, route_ids.T, route_logits,
        expert_gate, expert_up, expert_down,
    )


def solution(mesh):
    placed = (
        P("ep", None), P(), P(None, "tp"), P("tp", None, None), P("tp"), P("tp", None),
        P("ep", None), P(), P("ep", None), P("ep", None),
        P("ep", None, "tp"), P("ep", None, "tp"), P("ep", "tp", None),
    )
    return jax.shard_map(
        local, mesh=mesh, in_specs=placed, out_specs=(P("ep", "tp"), P("ep", "tp")), check_vma=False
    )
```

```python
import functools

import jax
import jax.numpy as jnp
from jax import lax
from jax.experimental import pallas as pl
from jax.experimental.pallas import tpu as pltpu
from jax.sharding import PartitionSpec as P

EPS = 1e-06
MESH = pl.DeviceIdType.MESH
F32, BF16 = jnp.float32, jnp.bfloat16


def ring_order(m):
    return [0] + sorted(range(1, m), key=lambda r: (-min(r, m - r), r))


def rms(values, gain):
    wide = values.astype(F32)
    inverse = lax.rsqrt(jnp.mean(wide * wide, axis=-1, keepdims=True) + EPS)
    return (wide * inverse * gain).astype(BF16)


def body(
    n, parts, cap,
    first_hbm, gains, inward_hbm, mixing, outward_hbm, x2, ids_t, logits_t,
    gate_hbm, up_hbm, down_hbm,
    out1, out2,
    first_v, inward_v, outward_v, gate_v, up_v, down_v, load_sem,
    normed, sent, portion, hidden, term, core_in, x_out, x_in, half_out, y_in, whole_out, back, total,
    halo_out, halo_in, extended, mixed, pooled, mix_term, mix_core, mix_x_out, mix_x_in,
    zs, zr, xs, xr, ds, dr, ys, yr,
    r1s, r1r, r2s, r2r, r3s, r3r, r4s, r4r, hs, hr, m1s, m1r, m2s, m2r,
):
    me = lax.axis_index("ep")
    t = lax.axis_index("tp")
    t_core = t + 1 - 2 * lax.rem(t, 2)
    t_x = lax.rem(t + 2, 4)
    t_diag = lax.rem(t_core + 2, 4)
    rows2, width = x2.shape
    w = width // parts
    m = n // 2
    a, b = me // 2, lax.rem(me, 2)
    me_y = 2 * a + 1 - b
    order = ring_order(m)
    groups = 4
    per = m // groups
    group_rows = 2 * per * cap
    rows1 = first_v.shape[0]
    tile1 = 128

    def quarter(index):
        return pl.ds(pl.multiple_of(index * w, w), w)

    def spot(i):
        return pl.ds(i * cap, cap)

    def group(g):
        return pl.ds(g * group_rows, group_rows)

    loads = [
        pltpu.make_async_copy(src, dst, load_sem.at[k])
        for k, (src, dst) in enumerate((
            (first_hbm, first_v), (inward_hbm, inward_v), (outward_hbm, outward_v),
            (gate_hbm.at[0], gate_v), (up_hbm.at[0], up_v), (down_hbm.at[0], down_v)))
    ]
    for load in loads:
        load.start()

    barrier = pltpu.get_barrier_semaphore()
    for r in range(1, m):
        pl.semaphore_signal(
            barrier, inc=1, device_id=(2 * lax.rem(a + r, m) + b, t), device_id_type=MESH)
    for step in (1, n - 1):
        pl.semaphore_signal(
            barrier, inc=1, device_id=(lax.rem(me + step, n), t), device_id_type=MESH)
    pl.semaphore_signal(barrier, inc=1, device_id=(me_y, t), device_id_type=MESH)
    for other in (t_core, t_x):
        pl.semaphore_signal(barrier, inc=1, device_id=(me, other), device_id_type=MESH)

    def remote(src, dst, ssem, rsem, ep, tp):
        return pltpu.make_async_remote_copy(
            src_ref=src, dst_ref=dst, send_sem=ssem, recv_sem=rsem,
            device_id=(ep, tp), device_id_type=MESH)

    def side(k, b_side):
        return spot(2 * k + b_side)

    def z_copy(k):
        return remote(sent.at[spot(k)], portion.at[side(k, 0), quarter(t)],
                      zs.at[k], zr.at[k], 2 * lax.rem(a + order[k], m) + b, t)

    def x_copy(k):
        piece = portion.at[side(k, 0), quarter(t)]
        return remote(piece, piece, xs.at[k], xr.at[k], me, t_x)

    def x_arrival(k):
        piece = portion.at[side(k, 0), quarter(t_x)]
        return remote(piece, piece, xs.at[k], xr.at[k], me, t_x)

    def y_copy(k, q):
        cols = quarter((t, t_x)[q])
        return remote(portion.at[side(k, 0), cols], portion.at[side(k, 1), cols],
                      ys.at[k, q], yr.at[k, q], me_y, t)

    def d_copy(k, b_side, q):
        piece = portion.at[side(k, b_side), quarter((t, t_x)[q])]
        return remote(piece, piece, ds.at[k, b_side, q], dr.at[k, b_side, q], me, t_core)

    def d_arrival(k, b_side, q):
        piece = portion.at[side(k, b_side), quarter((t_core, t_diag)[q])]
        return remote(piece, piece, ds.at[k, b_side, q], dr.at[k, b_side, q], me, t_core)

    def r1_copy(g, k):
        return remote(term.at[group(g), quarter((t_core, t_diag)[k])], core_in.at[k, group(g)],
                      r1s.at[g, k], r1r.at[g, k], me, t_core)

    def r2_copy(g):
        return remote(x_out.at[group(g)], x_in.at[group(g)], r2s.at[g], r2r.at[g], me, t_x)

    def r3_copy(k):
        return remote(half_out.at[side(k, 1)], y_in.at[spot(k)], r3s.at[k], r3r.at[k], me_y, t)

    def r4_copy(k):
        return remote(whole_out.at[spot(k)], back.at[spot(k)], r4s.at[k], r4r.at[k],
                      2 * lax.rem(a + m - order[k], m) + b, t)

    def m1_copy(k):
        return remote(mix_term.at[:, quarter((t_core, t_diag)[k])], mix_core.at[k],
                      m1s.at[k], m1r.at[k], me, t_core)

    def m2_copy():
        return remote(mix_x_out, mix_x_in, m2s, m2r, me, t_x)

    def halo_copy():
        return remote(halo_out, halo_in, hs, hr, lax.rem(me + 1, n), t)

    def norm_tile(j, carry):
        tile = pl.ds(pl.multiple_of(j * 64, 64), 64)
        normed[tile, :] = rms(x2[tile, :], gains[:, width:2 * width])
        return carry

    lax.fori_loop(0, rows2 // 64, norm_tile, None)

    before = (lax.broadcasted_iota(jnp.int32, (rows2, rows2), 0)
              < lax.broadcasted_iota(jnp.int32, (rows2, rows2), 1)).astype(BF16)
    places = lax.broadcasted_iota(jnp.int32, (cap, rows2), 0)

    def chosen(k):
        expert = lax.rem(a + order[k], m)
        named = (ids_t[0:1, :] == expert) | (ids_t[1:2, :] == expert)
        flags = jnp.broadcast_to(jnp.where(named, 1.0, 0.0), (16, rows2)).astype(BF16)
        slots = jnp.dot(flags, before, preferred_element_type=F32)[0:1, :].astype(jnp.int32)
        slots = jnp.where(named, slots, -1)
        return jnp.where(places == slots, 1.0, 0.0).astype(BF16)

    pl.semaphore_wait(barrier, m + 4)
    for k in range(1, m):
        sent[spot(k), :] = jnp.dot(
            chosen(k), normed[:, quarter(t)], preferred_element_type=F32).astype(BF16)
        z_copy(k).start()
    own_rows = chosen(0)
    for q in range(parts):
        portion[side(0, 0), q * w:(q + 1) * w] = jnp.dot(
            own_rows, normed[:, q * w:(q + 1) * w], preferred_element_type=F32).astype(BF16)
    y_copy(0, 0).start()
    y_copy(0, 1).start()

    loads[0].wait()
    loads[1].wait()

    def inward_tile(j, carry):
        tile = pl.ds(pl.multiple_of(j * tile1, tile1), tile1)
        later = pl.ds(pl.multiple_of(j * tile1 + 16, 16), tile1)
        rows = rms(first_v[tile, :], gains[:, 0:width])
        product = jnp.dot(rows, inward_v[...], preferred_element_type=F32).astype(BF16)
        extended[later, :] = product.astype(F32)
        return carry

    lax.fori_loop(0, rows1 // tile1, inward_tile, None)
    halo_out[...] = extended[rows1:rows1 + 16, :].astype(BF16)
    halo_copy().start()

    def members(g):
        return range(g * per, (g + 1) * per)

    def arrived(g):
        for k in members(g):
            if k > 0:
                z_copy(k).wait_recv()
                x_copy(k).start()
                y_copy(k, 0).start()
                d_copy(k, 0, 0).start()

    def over_y(g):
        for k in members(g):
            if k > 0:
                x_arrival(k).wait_recv()
                y_copy(k, 1).start()
                d_copy(k, 0, 1).start()

    def to_core(g):
        for k in members(g):
            for q in (0, 1):
                y_copy(k, q).wait_recv()
                d_copy(k, 1, q).start()

    def ready(g):
        for k in members(g):
            for b_side in (0, 1):
                if k > 0 or b_side > 0:
                    for q in (0, 1):
                        d_arrival(k, b_side, q).wait_recv()

    def compute(g):
        unit_tile = min(256, hidden.shape[1])

        def units(j, carry):
            cols = pl.ds(pl.multiple_of(j * unit_tile, unit_tile), unit_tile)
            gate = jnp.dot(portion[group(g), :], gate_v[:, cols], preferred_element_type=F32)
            up = jnp.dot(portion[group(g), :], up_v[:, cols], preferred_element_type=F32)
            hidden[:, cols] = (gate / (1.0 + jnp.exp(-gate)) * up).astype(BF16)
            return carry

        lax.fori_loop(0, hidden.shape[1] // unit_tile, units, None)

        def outs(j, carry):
            cols = quarter(j)
            term[group(g), cols] = jnp.dot(
                hidden[...], down_v[:, cols], preferred_element_type=F32).astype(BF16)
            return carry

        lax.fori_loop(0, parts, outs, None)
        for k in (1, 0):
            r1_copy(g, k).start()

    def over_x(g):
        r1_copy(g, 1).wait_recv()
        x_out[group(g), :] = (term[group(g), quarter(t_x)].astype(F32)
                              + core_in[1, group(g), :].astype(F32)).astype(BF16)
        r2_copy(g).start()

    def home(g):
        r1_copy(g, 0).wait_recv()
        r2_copy(g).wait_recv()
        half_out[group(g), :] = (term[group(g), quarter(t)].astype(F32)
                                 + core_in[0, group(g), :].astype(F32)
                                 + x_in[group(g), :].astype(F32)).astype(BF16)
        for k in members(g):
            r3_copy(k).start()

    def onward(g):
        for k in members(g):
            r3_copy(k).wait_recv()
            whole_out[spot(k), :] = (half_out[side(k, 0), :].astype(F32)
                                     + y_in[spot(k), :].astype(F32)).astype(BF16)
            if k > 0:
                r4_copy(k).start()

    arrived(1)

    halo_copy().wait_recv()
    loads[2].wait()
    extended[0:16, :] = jnp.where(me == 0, 0.0, halo_in[...].astype(F32))
    lanes = min(128, extended.shape[1])
    counts = jnp.minimum(
        me * rows1 + 1 + lax.broadcasted_iota(jnp.int32, (rows1, lanes), 0),
        jnp.left_shift(jnp.int32(2), t)).astype(F32)
    for c in range(extended.shape[1] // lanes):
        cols = slice(c * lanes, (c + 1) * lanes)
        whole = extended[:, cols]
        running, picked = whole, whole
        for level in range(4):
            running = running + pltpu.roll(running, 1 << level, 0)
            picked = jnp.where(t >= level, running, picked)
        mixed[:, cols] = (picked[16:, :] / counts - whole[16:, :]).astype(BF16)
    pooled[...] = (jnp.dot(mixed[...], mixing[0], preferred_element_type=F32)
                   * gains[:, 2 * width:]).astype(BF16)

    def outward_tile(j, carry):
        mix_term[:, quarter(j)] = jnp.dot(
            pooled[...], outward_v[:, quarter(j)], preferred_element_type=F32).astype(BF16)
        return carry

    lax.fori_loop(0, parts, outward_tile, None)
    m1_copy(1).start()
    m1_copy(0).start()

    to_core(0)
    arrived(2)
    over_y(1)
    m1_copy(1).wait_recv()
    mix_x_out[...] = (mix_term[:, quarter(t_x)].astype(F32)
                      + mix_core[1].astype(F32)).astype(BF16)
    m2_copy().start()
    for k in (3, 4, 5):
        loads[k].wait()
    arrived(3)
    ready(0)
    compute(0)
    over_y(2)
    over_y(3)
    to_core(1)
    over_x(0)
    ready(1)
    compute(1)
    to_core(2)
    over_x(1)
    home(0)
    ready(2)
    compute(2)
    to_core(3)
    over_x(2)
    home(1)
    ready(3)
    compute(3)
    over_x(3)
    onward(0)
    onward(1)
    home(2)
    onward(2)

    m1_copy(0).wait_recv()
    m2_copy().wait_recv()
    out1[...] = (mix_term[:, quarter(t)].astype(F32) + mix_core[0].astype(F32)
                 + mix_x_in[...].astype(F32)).astype(BF16)

    after = (lax.broadcasted_iota(jnp.int32, (rows2, rows2), 1)
             < lax.broadcasted_iota(jnp.int32, (rows2, rows2), 0)).astype(BF16)
    tall = lax.broadcasted_iota(jnp.int32, (rows2, cap), 1)
    difference = logits_t[0:1, :] - logits_t[1:2, :]
    lines = lax.broadcasted_iota(jnp.int32, (128, rows2), 0)
    listed = jnp.where(lines == 0, ids_t[0:1, :].astype(F32), ids_t[1:2, :].astype(F32))
    listed = jnp.where(lines == 2, 1.0 / (1.0 + jnp.exp(-difference)), listed)
    listed = jnp.where(lines == 3, 1.0 / (1.0 + jnp.exp(difference)), listed)
    listed = listed.T

    def combine(k, source):
        expert = lax.rem(a + order[k], m).astype(F32)
        is0, is1 = listed[:, 0:1] == expert, listed[:, 1:2] == expert
        named = is0 | is1
        flags = jnp.broadcast_to(jnp.where(named, 1.0, 0.0), (rows2, 128)).astype(BF16)
        slots = jnp.dot(after, flags, preferred_element_type=F32)[:, 0:1].astype(jnp.int32)
        slots = jnp.where(named, slots, -1)
        table = jnp.where(tall == slots, 1.0, 0.0).astype(BF16)
        share = jnp.where(is0, listed[:, 2:3], jnp.where(is1, listed[:, 3:4], 0.0))
        picked = share * jnp.dot(table, source[spot(k), :], preferred_element_type=F32)
        if k == 0:
            total[...] = picked
        else:
            total[...] += picked

    def gather(g):
        for k in members(g):
            if k > 0:
                r4_copy(k).wait_recv()
            combine(k, back if k > 0 else whole_out)

    gather(0)
    home(3)
    gather(1)
    onward(3)
    gather(2)
    gather(3)
    out2[...] = total[...].astype(BF16)

    for k in range(m):
        for q in (0, 1):
            y_copy(k, q).wait_send()
            d_copy(k, 1, q).wait_send()
            if k > 0:
                d_copy(k, 0, q).wait_send()
        r3_copy(k).wait_send()
        if k > 0:
            z_copy(k).wait_send()
            x_copy(k).wait_send()
            r4_copy(k).wait_send()
    for g in range(groups):
        r1_copy(g, 0).wait_send()
        r1_copy(g, 1).wait_send()
        r2_copy(g).wait_send()
    m1_copy(0).wait_send()
    m1_copy(1).wait_send()
    m2_copy().wait_send()
    halo_copy().wait_send()


def local(
    first_input, first_gain, pool_inward, pool_mixing, pool_scale, pool_outward,
    second_input, second_gain, route_ids, route_logits, expert_gate, expert_up, expert_down,
):
    n = lax.axis_size("ep")
    parts = lax.axis_size("tp")
    m = n // 2
    rows1, width = first_input.shape
    rows2 = second_input.shape[0]
    w = width // parts
    cap = 2 * rows2 * 9 // (8 * m)
    cap = -(-cap // 16) * 16
    channels = pool_inward.shape[1]
    units = expert_gate.shape[2]
    slots = n * cap
    gains = lax.optimization_barrier(
        jnp.concatenate([first_gain, second_gain, pool_scale]).astype(F32))[None, :]
    dma = pltpu.SemaphoreType.DMA
    vmem = pl.BlockSpec(memory_space=pltpu.VMEM)
    anywhere = pl.BlockSpec(memory_space=pl.ANY)
    v = pltpu.VMEM
    scratch = [
        v((rows1, width), BF16), v((width, channels), BF16), v((channels, width), BF16),
        v((width, units), BF16), v((width, units), BF16), v((units, width), BF16), dma((6,)),
        v((rows2, width), BF16), v((slots // 2, w), BF16), v((slots, width), BF16),
        v((slots // 4, units), BF16), v((slots, width), BF16), v((2, slots, w), BF16),
        v((slots, w), BF16), v((slots, w), BF16), v((slots, w), BF16), v((slots // 2, w), BF16),
        v((slots // 2, w), BF16), v((slots // 2, w), BF16),
        v((rows2, w), F32),
        v((16, channels), BF16), v((16, channels), BF16), v((rows1 + 16, channels), F32),
        v((rows1, channels), BF16), v((rows1, channels), BF16), v((rows1, width), BF16),
        v((2, rows1, w), BF16), v((rows1, w), BF16), v((rows1, w), BF16),
        dma((m,)), dma((m,)), dma((m,)), dma((m,)),
        dma((m, 2, 2)), dma((m, 2, 2)), dma((m, 2)), dma((m, 2)),
        dma((4, 2)), dma((4, 2)), dma((4,)), dma((4,)), dma((m,)), dma((m,)), dma((m,)), dma((m,)),
        dma(()), dma(()), dma((2,)), dma((2,)), dma(()), dma(()),
    ]
    return pl.pallas_call(
        functools.partial(body, n, parts, cap),
        out_shape=(jax.ShapeDtypeStruct((rows1, w), BF16), jax.ShapeDtypeStruct((rows2, w), BF16)),
        in_specs=[anywhere, vmem, anywhere, vmem, anywhere, vmem, vmem, vmem,
                  anywhere, anywhere, anywhere],
        out_specs=(vmem, vmem),
        scratch_shapes=scratch,
        compiler_params=pltpu.CompilerParams(
            collective_id=0, has_side_effects=True, vmem_limit_bytes=60 * 1024 * 1024),
    )(
        first_input, gains, pool_inward, pool_mixing, pool_outward, second_input,
        route_ids.T, route_logits.T, expert_gate, expert_up, expert_down,
    )


def solution(mesh):
    placed = (
        P("ep", None), P(), P(None, "tp"), P("tp", None, None), P("tp"), P("tp", None),
        P("ep", None), P(), P("ep", None), P("ep", None),
        P("ep", None, "tp"), P("ep", None, "tp"), P("ep", "tp", None),
    )
    return jax.shard_map(
        local, mesh=mesh, in_specs=placed, out_specs=(P("ep", "tp"), P("ep", "tp")), check_vma=False
    )
```

```python
import functools

import jax
import jax.numpy as jnp
from jax import lax
from jax.experimental import pallas as pl
from jax.experimental.pallas import tpu as pltpu
from jax.sharding import PartitionSpec as P

EPS = 1e-06
MESH = pl.DeviceIdType.MESH
F32, BF16 = jnp.float32, jnp.bfloat16


def ring_order(m):
    return [0] + sorted(range(1, m), key=lambda r: (-min(r, m - r), r))


def rms(values, gain):
    wide = values.astype(F32)
    inverse = lax.rsqrt(jnp.mean(wide * wide, axis=-1, keepdims=True) + EPS)
    return (wide * inverse * gain).astype(BF16)


def body(
    n, parts, cap,
    first_hbm, gains, inward_hbm, mixing, outward_hbm, x2, ids_t, logits_t,
    gate_hbm, up_hbm, down_hbm,
    out1, out2,
    first_v, inward_v, outward_v, gate_v, up_v, down_v, load_sem,
    normed, sent, portion, hidden, term, core_in, x_out, x_in, half_out, y_in, whole_out, back, total,
    halo_out, halo_in, extended, mixed, pooled, mix_term, mix_core, mix_x_out, mix_x_in,
    zs, zr, xs, xr, ds, dr, ys, yr,
    r1s, r1r, r2s, r2r, r3s, r3r, r4s, r4r, hs, hr, m1s, m1r, m2s, m2r,
):
    me = lax.axis_index("ep")
    t = lax.axis_index("tp")
    t_core = t + 1 - 2 * lax.rem(t, 2)
    t_x = lax.rem(t + 2, 4)
    t_diag = lax.rem(t_core + 2, 4)
    rows2, width = x2.shape
    w = width // parts
    m = n // 2
    a, b = me // 2, lax.rem(me, 2)
    me_y = 2 * a + 1 - b
    order = ring_order(m)
    groups = 4
    per = m // groups
    group_rows = 2 * per * cap
    rows1 = first_v.shape[0]
    tile1 = 128

    def quarter(index):
        return pl.ds(pl.multiple_of(index * w, w), w)

    def spot(i):
        return pl.ds(i * cap, cap)

    def group(g):
        return pl.ds(g * group_rows, group_rows)

    loads = [
        pltpu.make_async_copy(src, dst, load_sem.at[k])
        for k, (src, dst) in enumerate((
            (first_hbm, first_v), (inward_hbm, inward_v), (outward_hbm, outward_v),
            (gate_hbm.at[0], gate_v), (up_hbm.at[0], up_v), (down_hbm.at[0], down_v)))
    ]
    for load in loads:
        load.start()

    barrier = pltpu.get_barrier_semaphore()
    for r in range(1, m):
        pl.semaphore_signal(
            barrier, inc=1, device_id=(2 * lax.rem(a + r, m) + b, t), device_id_type=MESH)
    for step in (1, n - 1):
        pl.semaphore_signal(
            barrier, inc=1, device_id=(lax.rem(me + step, n), t), device_id_type=MESH)
    pl.semaphore_signal(barrier, inc=1, device_id=(me_y, t), device_id_type=MESH)
    for other in (t_core, t_x):
        pl.semaphore_signal(barrier, inc=1, device_id=(me, other), device_id_type=MESH)

    def remote(src, dst, ssem, rsem, ep, tp):
        return pltpu.make_async_remote_copy(
            src_ref=src, dst_ref=dst, send_sem=ssem, recv_sem=rsem,
            device_id=(ep, tp), device_id_type=MESH)

    def side(k, b_side):
        return spot(2 * k + b_side)

    def z_copy(k):
        return remote(sent.at[spot(k)], portion.at[side(k, 0), quarter(t)],
                      zs.at[k], zr.at[k], 2 * lax.rem(a + order[k], m) + b, t)

    def x_copy(k):
        piece = portion.at[side(k, 0), quarter(t)]
        return remote(piece, piece, xs.at[k], xr.at[k], me, t_x)

    def x_arrival(k):
        piece = portion.at[side(k, 0), quarter(t_x)]
        return remote(piece, piece, xs.at[k], xr.at[k], me, t_x)

    def y_copy(k, q):
        cols = quarter((t, t_x)[q])
        return remote(portion.at[side(k, 0), cols], portion.at[side(k, 1), cols],
                      ys.at[k, q], yr.at[k, q], me_y, t)

    def d_copy(k, b_side, q):
        piece = portion.at[side(k, b_side), quarter((t, t_x)[q])]
        return remote(piece, piece, ds.at[k, b_side, q], dr.at[k, b_side, q], me, t_core)

    def d_arrival(k, b_side, q):
        piece = portion.at[side(k, b_side), quarter((t_core, t_diag)[q])]
        return remote(piece, piece, ds.at[k, b_side, q], dr.at[k, b_side, q], me, t_core)

    def r1_copy(g, k):
        return remote(term.at[group(g), quarter((t_core, t_diag)[k])], core_in.at[k, group(g)],
                      r1s.at[g, k], r1r.at[g, k], me, t_core)

    def r2_copy(k, b_side):
        rows = side(k, b_side)
        return remote(x_out.at[rows], x_in.at[rows], r2s.at[k, b_side], r2r.at[k, b_side], me, t_x)

    def r3_copy(k):
        return remote(half_out.at[spot(k)], y_in.at[spot(k)], r3s.at[k], r3r.at[k], me_y, t)

    def r4_copy(k):
        return remote(whole_out.at[spot(k)], back.at[spot(k)], r4s.at[k], r4r.at[k],
                      2 * lax.rem(a + m - order[k], m) + b, t)

    def m1_copy(k):
        return remote(mix_term.at[:, quarter((t_core, t_diag)[k])], mix_core.at[k],
                      m1s.at[k], m1r.at[k], me, t_core)

    def m2_copy():
        return remote(mix_x_out, mix_x_in, m2s, m2r, me, t_x)

    def halo_copy():
        return remote(halo_out, halo_in, hs, hr, lax.rem(me + 1, n), t)

    def norm_tile(j, carry):
        tile = pl.ds(pl.multiple_of(j * 64, 64), 64)
        normed[tile, :] = rms(x2[tile, :], gains[:, width:2 * width])
        return carry

    lax.fori_loop(0, rows2 // 64, norm_tile, None)

    before = (lax.broadcasted_iota(jnp.int32, (rows2, rows2), 0)
              < lax.broadcasted_iota(jnp.int32, (rows2, rows2), 1)).astype(BF16)
    places = lax.broadcasted_iota(jnp.int32, (cap, rows2), 0)

    def chosen(k):
        expert = lax.rem(a + order[k], m)
        named = (ids_t[0:1, :] == expert) | (ids_t[1:2, :] == expert)
        flags = jnp.broadcast_to(jnp.where(named, 1.0, 0.0), (16, rows2)).astype(BF16)
        slots = jnp.dot(flags, before, preferred_element_type=F32)[0:1, :].astype(jnp.int32)
        slots = jnp.where(named, slots, -1)
        return jnp.where(places == slots, 1.0, 0.0).astype(BF16)

    pl.semaphore_wait(barrier, m + 4)
    for k in range(1, m):
        sent[spot(k), :] = jnp.dot(
            chosen(k), normed[:, quarter(t)], preferred_element_type=F32).astype(BF16)
        z_copy(k).start()
    own_rows = chosen(0)
    for q in range(parts):
        portion[side(0, 0), q * w:(q + 1) * w] = jnp.dot(
            own_rows, normed[:, q * w:(q + 1) * w], preferred_element_type=F32).astype(BF16)
    y_copy(0, 0).start()
    y_copy(0, 1).start()

    loads[0].wait()
    loads[1].wait()

    def inward_tile(j, carry):
        tile = pl.ds(pl.multiple_of(j * tile1, tile1), tile1)
        later = pl.ds(pl.multiple_of(j * tile1 + 16, 16), tile1)
        rows = rms(first_v[tile, :], gains[:, 0:width])
        product = jnp.dot(rows, inward_v[...], preferred_element_type=F32).astype(BF16)
        extended[later, :] = product.astype(F32)
        return carry

    lax.fori_loop(0, rows1 // tile1, inward_tile, None)
    halo_out[...] = extended[rows1:rows1 + 16, :].astype(BF16)
    halo_copy().start()

    def members(g):
        return range(g * per, (g + 1) * per)

    def arrived(g):
        for k in members(g):
            if k > 0:
                z_copy(k).wait_recv()
                x_copy(k).start()
                y_copy(k, 0).start()
                d_copy(k, 0, 0).start()

    def over_y(g):
        for k in members(g):
            if k > 0:
                x_arrival(k).wait_recv()
                y_copy(k, 1).start()
                d_copy(k, 0, 1).start()

    def to_core(g):
        for k in members(g):
            for q in (0, 1):
                y_copy(k, q).wait_recv()
                d_copy(k, 1, q).start()

    def ready(g):
        for k in members(g):
            for b_side in (0, 1):
                if k > 0 or b_side > 0:
                    for q in (0, 1):
                        d_arrival(k, b_side, q).wait_recv()

    def compute(g):
        unit_tile = min(256, hidden.shape[1])

        def units(j, carry):
            cols = pl.ds(pl.multiple_of(j * unit_tile, unit_tile), unit_tile)
            gate = jnp.dot(portion[group(g), :], gate_v[:, cols], preferred_element_type=F32)
            up = jnp.dot(portion[group(g), :], up_v[:, cols], preferred_element_type=F32)
            hidden[:, cols] = (gate / (1.0 + jnp.exp(-gate)) * up).astype(BF16)
            return carry

        lax.fori_loop(0, hidden.shape[1] // unit_tile, units, None)

        def outs(j, carry):
            cols = quarter(j)
            term[group(g), cols] = jnp.dot(
                hidden[...], down_v[:, cols], preferred_element_type=F32).astype(BF16)
            return carry

        lax.fori_loop(0, parts, outs, None)
        for k in (1, 0):
            r1_copy(g, k).start()

    def over_x(g):
        r1_copy(g, 1).wait_recv()
        for b_side in (1, 0):
            for k in members(g):
                rows = side(k, b_side)
                x_out[rows, :] = (term[rows, quarter(t_x)].astype(F32)
                                  + core_in[1, rows, :].astype(F32)).astype(BF16)
                r2_copy(k, b_side).start()

    def half_sum(k, b_side):
        rows = side(k, b_side)
        return (term[rows, quarter(t)].astype(F32) + core_in[0, rows, :].astype(F32)
                + x_in[rows, :].astype(F32))

    def home(g):
        r1_copy(g, 0).wait_recv()
        for k in members(g):
            r2_copy(k, 1).wait_recv()
            half_out[spot(k), :] = half_sum(k, 1).astype(BF16)
            r3_copy(k).start()

    def onward(g):
        for k in members(g):
            r2_copy(k, 0).wait_recv()
            r3_copy(k).wait_recv()
            whole_out[spot(k), :] = (half_sum(k, 0) + y_in[spot(k), :].astype(F32)).astype(BF16)
            if k > 0:
                r4_copy(k).start()

    arrived(1)

    halo_copy().wait_recv()
    loads[2].wait()
    extended[0:16, :] = jnp.where(me == 0, 0.0, halo_in[...].astype(F32))
    lanes = min(128, extended.shape[1])
    counts = jnp.minimum(
        me * rows1 + 1 + lax.broadcasted_iota(jnp.int32, (rows1, lanes), 0),
        jnp.left_shift(jnp.int32(2), t)).astype(F32)
    for c in range(extended.shape[1] // lanes):
        cols = slice(c * lanes, (c + 1) * lanes)
        whole = extended[:, cols]
        running, picked = whole, whole
        for level in range(4):
            running = running + pltpu.roll(running, 1 << level, 0)
            picked = jnp.where(t >= level, running, picked)
        mixed[:, cols] = (picked[16:, :] / counts - whole[16:, :]).astype(BF16)
    pooled[...] = (jnp.dot(mixed[...], mixing[0], preferred_element_type=F32)
                   * gains[:, 2 * width:]).astype(BF16)

    def outward_tile(j, carry):
        mix_term[:, quarter(j)] = jnp.dot(
            pooled[...], outward_v[:, quarter(j)], preferred_element_type=F32).astype(BF16)
        return carry

    lax.fori_loop(0, parts, outward_tile, None)
    m1_copy(1).start()
    m1_copy(0).start()

    to_core(0)
    arrived(2)
    over_y(1)
    m1_copy(1).wait_recv()
    mix_x_out[...] = (mix_term[:, quarter(t_x)].astype(F32)
                      + mix_core[1].astype(F32)).astype(BF16)
    m2_copy().start()
    for k in (3, 4, 5):
        loads[k].wait()
    arrived(3)
    ready(0)
    compute(0)
    over_y(2)
    over_y(3)
    to_core(1)
    over_x(0)
    ready(1)
    compute(1)
    to_core(2)
    over_x(1)
    home(0)
    ready(2)
    compute(2)
    to_core(3)
    over_x(2)
    home(1)
    ready(3)
    compute(3)
    over_x(3)
    onward(0)
    onward(1)
    home(2)
    home(3)
    onward(2)

    m1_copy(0).wait_recv()
    m2_copy().wait_recv()
    out1[...] = (mix_term[:, quarter(t)].astype(F32) + mix_core[0].astype(F32)
                 + mix_x_in[...].astype(F32)).astype(BF16)

    after = (lax.broadcasted_iota(jnp.int32, (rows2, rows2), 1)
             < lax.broadcasted_iota(jnp.int32, (rows2, rows2), 0)).astype(BF16)
    tall = lax.broadcasted_iota(jnp.int32, (rows2, cap), 1)
    difference = logits_t[0:1, :] - logits_t[1:2, :]
    lines = lax.broadcasted_iota(jnp.int32, (128, rows2), 0)
    listed = jnp.where(lines == 0, ids_t[0:1, :].astype(F32), ids_t[1:2, :].astype(F32))
    listed = jnp.where(lines == 2, 1.0 / (1.0 + jnp.exp(-difference)), listed)
    listed = jnp.where(lines == 3, 1.0 / (1.0 + jnp.exp(difference)), listed)
    listed = listed.T

    def combine(k, source):
        expert = lax.rem(a + order[k], m).astype(F32)
        is0, is1 = listed[:, 0:1] == expert, listed[:, 1:2] == expert
        named = is0 | is1
        flags = jnp.broadcast_to(jnp.where(named, 1.0, 0.0), (rows2, 128)).astype(BF16)
        slots = jnp.dot(after, flags, preferred_element_type=F32)[:, 0:1].astype(jnp.int32)
        slots = jnp.where(named, slots, -1)
        table = jnp.where(tall == slots, 1.0, 0.0).astype(BF16)
        share = jnp.where(is0, listed[:, 2:3], jnp.where(is1, listed[:, 3:4], 0.0))
        picked = share * jnp.dot(table, source[spot(k), :], preferred_element_type=F32)
        if k == 0:
            total[...] = picked
        else:
            total[...] += picked

    def gather(g):
        for k in members(g):
            if k > 0:
                r4_copy(k).wait_recv()
            combine(k, back if k > 0 else whole_out)

    gather(0)
    onward(3)
    gather(1)
    gather(2)
    gather(3)
    out2[...] = total[...].astype(BF16)

    for k in range(m):
        for q in (0, 1):
            y_copy(k, q).wait_send()
            d_copy(k, 1, q).wait_send()
            if k > 0:
                d_copy(k, 0, q).wait_send()
        r3_copy(k).wait_send()
        r2_copy(k, 0).wait_send()
        r2_copy(k, 1).wait_send()
        if k > 0:
            z_copy(k).wait_send()
            x_copy(k).wait_send()
            r4_copy(k).wait_send()
    for g in range(groups):
        r1_copy(g, 0).wait_send()
        r1_copy(g, 1).wait_send()
    m1_copy(0).wait_send()
    m1_copy(1).wait_send()
    m2_copy().wait_send()
    halo_copy().wait_send()


def local(
    first_input, first_gain, pool_inward, pool_mixing, pool_scale, pool_outward,
    second_input, second_gain, route_ids, route_logits, expert_gate, expert_up, expert_down,
):
    n = lax.axis_size("ep")
    parts = lax.axis_size("tp")
    m = n // 2
    rows1, width = first_input.shape
    rows2 = second_input.shape[0]
    w = width // parts
    cap = 2 * rows2 * 9 // (8 * m)
    cap = -(-cap // 16) * 16
    channels = pool_inward.shape[1]
    units = expert_gate.shape[2]
    slots = n * cap
    gains = lax.optimization_barrier(
        jnp.concatenate([first_gain, second_gain, pool_scale]).astype(F32))[None, :]
    dma = pltpu.SemaphoreType.DMA
    vmem = pl.BlockSpec(memory_space=pltpu.VMEM)
    anywhere = pl.BlockSpec(memory_space=pl.ANY)
    v = pltpu.VMEM
    scratch = [
        v((rows1, width), BF16), v((width, channels), BF16), v((channels, width), BF16),
        v((width, units), BF16), v((width, units), BF16), v((units, width), BF16), dma((6,)),
        v((rows2, width), BF16), v((slots // 2, w), BF16), v((slots, width), BF16),
        v((slots // 4, units), BF16), v((slots, width), BF16), v((2, slots, w), BF16),
        v((slots, w), BF16), v((slots, w), BF16), v((slots // 2, w), BF16), v((slots // 2, w), BF16),
        v((slots // 2, w), BF16), v((slots // 2, w), BF16),
        v((rows2, w), F32),
        v((16, channels), BF16), v((16, channels), BF16), v((rows1 + 16, channels), F32),
        v((rows1, channels), BF16), v((rows1, channels), BF16), v((rows1, width), BF16),
        v((2, rows1, w), BF16), v((rows1, w), BF16), v((rows1, w), BF16),
        dma((m,)), dma((m,)), dma((m,)), dma((m,)),
        dma((m, 2, 2)), dma((m, 2, 2)), dma((m, 2)), dma((m, 2)),
        dma((4, 2)), dma((4, 2)), dma((m, 2)), dma((m, 2)), dma((m,)), dma((m,)), dma((m,)), dma((m,)),
        dma(()), dma(()), dma((2,)), dma((2,)), dma(()), dma(()),
    ]
    return pl.pallas_call(
        functools.partial(body, n, parts, cap),
        out_shape=(jax.ShapeDtypeStruct((rows1, w), BF16), jax.ShapeDtypeStruct((rows2, w), BF16)),
        in_specs=[anywhere, vmem, anywhere, vmem, anywhere, vmem, vmem, vmem,
                  anywhere, anywhere, anywhere],
        out_specs=(vmem, vmem),
        scratch_shapes=scratch,
        compiler_params=pltpu.CompilerParams(
            collective_id=0, has_side_effects=True, vmem_limit_bytes=60 * 1024 * 1024),
    )(
        first_input, gains, pool_inward, pool_mixing, pool_outward, second_input,
        route_ids.T, route_logits.T, expert_gate, expert_up, expert_down,
    )


def solution(mesh):
    placed = (
        P("ep", None), P(), P(None, "tp"), P("tp", None, None), P("tp"), P("tp", None),
        P("ep", None), P(), P("ep", None), P("ep", None),
        P("ep", None, "tp"), P("ep", None, "tp"), P("ep", "tp", None),
    )
    return jax.shard_map(
        local, mesh=mesh, in_specs=placed, out_specs=(P("ep", "tp"), P("ep", "tp")), check_vma=False
    )
```
